32 devices in a mesh: kv: 8 (over z, x), tp: 4 (over y, core).
Axes of the slice: x: 2, y: 2, z: 4, core: 2. Of those that a mesh axis runs over, the one named last changes fastest.
Arguments:
- tokens: bfloat16 [384, 4096], P(None, ('kv', 'tp')), may hold values from -90 to 90
- norm_gain: float32 [4096], P('kv'), may hold values from 0.1 to 1.9
- w_query: bfloat16 [4096, 2048], P('kv', 'tp'), may hold values from -0.09375 to 0.09375
- w_key: bfloat16 [4096, 2048], P('kv', 'tp'), may hold values from -0.09375 to 0.09375
- w_value: bfloat16 [4096, 2048], P('kv', 'tp'), may hold values from -0.09375 to 0.09375
- w_outgate: bfloat16 [4096, 2048], P('kv', 'tp'), may hold values from -0.09375 to 0.09375
- w_igate: bfloat16 [4096, 16], replicated, may hold values from -0.09375 to 0.09375
- w_fgate: bfloat16 [4096, 16], replicated, may hold values from -0.09375 to 0.09375
- forget_bias: float32 [16], P('tp'), may hold values from -1 to 5
- head_gain: float32 [2048], P('tp'), may hold values from 0.1 to 1.9
- w_proj: bfloat16 [2048, 4096], P('tp', 'kv'), may hold values from -0.125 to 0.125
- mixer_gain: float32 [4096], P('kv'), may hold values from 0.1 to 1.9
- w_gate: bfloat16 [4096, 11264], P('kv', 'tp'), may hold values from -0.09375 to 0.09375
- w_up: bfloat16 [4096, 11264], P('kv', 'tp'), may hold values from -0.09375 to 0.09375
- w_down: bfloat16 [11264, 4096], P('tp', 'kv'), may hold values from -0.0546875 to 0.0546875
- state_c: float32 [384, 16, 128, 128], P('kv', 'tp'), may hold values from -0.5 to 0.5
- state_m: float32 [384, 16], P('kv', 'tp'), may hold values from -4 to 4
- tail_keys: bfloat16 [384, 16, 64, 128], P('kv', 'tp'), may hold values from -6 to 6
- tail_values: bfloat16 [384, 16, 64, 128], P('kv', 'tp'), may hold values from -6 to 6
- tail_gate: float32 [384, 16, 64], P('kv', 'tp'), may hold values from -8 to 130
- block_forget: float32 [384, 16], P('kv', 'tp'), may hold values from -6 to 0
- lengths: int32 [384], P('kv'), may hold values from 1 to 64, 6144 in all
Outputs:
- result: bfloat16 [384, 4096], P(None, ('kv', 'tp'))
The draws below stay inside these ranges and needn't reach their ends.
All inputs are finite; a program needn't handle non-finite values. No bound on the sum of `lengths` on one device may be relied on, other than what follows from the above.
Results may differ from the reference program's by a relative error of at most 0.012.
Values may be sent and summed in bfloat16 or wider, within the bound.
A program may use at most 128 MiB of HBM per device.

```python
import math
import jax
import jax.numpy as jnp
import numpy as np
from jax import lax

D = 4096
HEADS = 16
DH = 128
FF = 11264
SPAN = 64
SEQS = 384
N_TP = 4


def draw_tokens(key, part):
    first, second = jax.random.split(key, 2)
    columns = jnp.arange(D, dtype=jnp.float32) / D
    rough = jax.random.uniform(second, (D,), jnp.float32, 0.6, 1.6)
    scale = 0.4 * 10.0 ** columns * rough
    base = jnp.clip(jax.random.normal(first, (SEQS, D), jnp.float32), -4.0, 4.0)
    values = base * scale
    return values.astype(jnp.bfloat16)


def draw_tail_gate(key, part):
    first = jax.random.fold_in(key, 0)
    base = jnp.clip(jax.random.normal(first, (SEQS, HEADS, SPAN), jnp.float32) * 1.5 - 1.0, -8.0, 6.0)
    return base


def shard_levels(own_key, extent, shards, smallest, high):
    gain, own = 1.0, jax.random.fold_in(own_key, 6)
    for dim, shards_of in shards:
        steps = jnp.exp(jax.random.uniform(jax.random.fold_in(own, dim), (shards_of,), jnp.float32, smallest / len(shards), high / len(shards)))
        gain = gain * jnp.repeat(steps, extent[dim] // shards_of).reshape([-1 if axis == dim else 1 for axis in range(len(extent))])
    return gain


def length_profile(count, total, limit, lean):
    weights = [(1 << 20) // math.isqrt(rank ** lean) + 1 for rank in range(2, count + 1)]
    surplus, counts = total - limit - (count - 1), [1] * (count - 1)
    while surplus > 0:
        candidates = [i for i in range(count - 1) if counts[i] < limit]
        pool, left = sum([weights[i] for i in candidates]), surplus
        for i in candidates:
            more = min(limit - counts[i], max(1, left * weights[i] // pool), surplus)
            counts[i] = counts[i] + more
            surplus = surplus - more
    return np.array([limit] + counts)


def uneven_parts(own_key, count, total, limit, lean):
    if count == 2:
        one = jax.random.randint(own_key, (), max(1, total - limit), min(limit, total - 1) + 1)
        return jnp.stack([one, total - one])
    sizes = jnp.asarray(length_profile(count, total, limit, lean), jnp.int32)
    twos = (count - 1) // 2
    giver, taker = sizes[1:1 + 2 * twos:2], sizes[2:2 + 2 * twos:2]
    room = jnp.minimum(giver - 1, limit - taker)
    moved = jax.random.randint(jax.random.fold_in(own_key, 1), (twos,), 0, 1 << 20) % (room + 1)
    sizes = sizes.at[1:1 + 2 * twos:2].set(giver - moved).at[2:2 + 2 * twos:2].set(taker + moved)
    return sizes[jax.random.permutation(jax.random.fold_in(own_key, 2), count)]


def bell_draw(key, shape, spread, bound, pieces=(), kind=jnp.bfloat16):
    entries = spread * jax.random.normal(key, shape, jnp.float32)
    if pieces:
        entries = entries * shard_levels(key, shape, pieces, -0.22, 0.18)
    return jnp.clip(entries, -bound, bound).astype(kind)


def setup_inputs(seed: int = 0) -> dict:
    arg_keys = jax.random.split(jax.random.key(seed), 23)
    tokens = draw_tokens(jax.random.fold_in(arg_keys[22], 71), 0)
    norm_gain = jnp.clip(1.0 + 0.18 * jax.random.normal(arg_keys[1], (D,), jnp.float32), 0.1, 1.9)
    w_query = bell_draw(arg_keys[2], (D, HEADS * DH), D ** -0.5, 0.09375, ((0, 8), (1, 4)))
    w_key = bell_draw(arg_keys[3], (D, HEADS * DH), D ** -0.5, 0.09375, ((0, 8), (1, 4)))
    w_value = bell_draw(arg_keys[4], (D, HEADS * DH), D ** -0.5, 0.09375, ((0, 8), (1, 4)))
    w_outgate = bell_draw(arg_keys[5], (D, HEADS * DH), D ** -0.5, 0.09375, ((0, 8), (1, 4)))
    w_igate = bell_draw(arg_keys[6], (D, HEADS), D ** -0.5, 0.09375)
    w_fgate = bell_draw(arg_keys[7], (D, HEADS), D ** -0.5, 0.09375)
    forget_bias = jnp.clip(-1.0 + 6.0 * jax.random.uniform(arg_keys[8], (HEADS,), jnp.float32) ** shard_levels(arg_keys[8], (HEADS,), ((0, 4),), -0.2, 0.2), -1.0, 5.0)
    head_gain = jnp.clip(1.0 + 0.18 * jax.random.normal(arg_keys[9], (HEADS * DH,), jnp.float32), 0.1, 1.9)
    w_proj = bell_draw(arg_keys[10], (HEADS * DH, D), (HEADS * DH) ** -0.5, 0.125, ((0, 4), (1, 8)))
    mixer_gain = jnp.clip(1.0 + 0.18 * jax.random.normal(arg_keys[11], (D,), jnp.float32), 0.1, 1.9)
    w_gate = bell_draw(arg_keys[12], (D, FF), D ** -0.5, 0.09375, ((0, 8), (1, 4)))
    w_up = bell_draw(arg_keys[13], (D, FF), D ** -0.5, 0.09375, ((0, 8), (1, 4)))
    w_down = bell_draw(arg_keys[14], (FF, D), FF ** -0.5, 0.0546875, ((0, 4), (1, 8)))
    state_c = bell_draw(arg_keys[15], (SEQS, HEADS, DH, DH), DH ** -0.5, 0.5, ((0, 8), (1, 4)), jnp.float32)
    state_m = bell_draw(arg_keys[16], (SEQS, HEADS), 1.0, 4.0, ((0, 8), (1, 4)), jnp.float32)
    tail_keys = bell_draw(arg_keys[17], (SEQS, HEADS, SPAN, DH), 1.0, 6.0, ((0, 8), (1, 4)))
    tail_values = bell_draw(arg_keys[18], (SEQS, HEADS, SPAN, DH), 1.0, 6.0, ((0, 8), (1, 4)))
    tail_gate = draw_tail_gate(jax.random.fold_in(arg_keys[22], 71), 0)
    block_forget = jnp.clip(-6.0 + 6.0 * jax.random.uniform(arg_keys[20], (SEQS, HEADS), jnp.float32) ** shard_levels(arg_keys[20], (SEQS, HEADS), ((0, 8), (1, 4)), -0.2, 0.2), -6.0, 0.0)
    lengths = uneven_parts(arg_keys[21], SEQS, SEQS * SPAN // 4, SPAN, 2).astype(jnp.int32)
    return dict(tokens=tokens, norm_gain=norm_gain, w_query=w_query, w_key=w_key, w_value=w_value, w_outgate=w_outgate, w_igate=w_igate, w_fgate=w_fgate, forget_bias=forget_bias, head_gain=head_gain, w_proj=w_proj, mixer_gain=mixer_gain, w_gate=w_gate, w_up=w_up, w_down=w_down, state_c=state_c, state_m=state_m, tail_keys=tail_keys, tail_values=tail_values, tail_gate=tail_gate, block_forget=block_forget, lengths=lengths)


EPS = 1e-06

def recall(query, key, value, igate, fpre, state_c, state_m, tail_keys, tail_values, tail_gate, block_forget, lengths):
    f32 = jnp.float32
    span = tail_keys.shape[2]
    head_dim = query.shape[2]
    running = block_forget + jax.nn.log_sigmoid(fpre)
    inter = running + state_m
    live = jnp.arange(span, dtype=jnp.int32)[None, :] < lengths[:, None]
    tail_log = jnp.where(live[:, None, :], running[:, :, None] + tail_gate, -jnp.inf)
    top = jnp.maximum(jnp.maximum(inter, lax.optimization_barrier(jnp.max(tail_log, axis=2))), igate)
    w_inter = jnp.exp(inter - top)
    w_tail = jnp.exp(tail_log - top[:, :, None])
    w_own = jnp.exp(igate - top)
    scores = jnp.einsum('shpd,shd->shp', tail_keys.astype(f32), query) * head_dim ** (-0.5)
    own = lax.optimization_barrier(jnp.sum(query * key, axis=2))
    memory = jnp.einsum('shvk,shk->shv', state_c, query)
    weighted = w_tail * scores
    return w_inter[:, :, None] * memory + jnp.einsum('shp,shpv->shv', weighted, tail_values.astype(f32)) + (w_own * own)[:, :, None] * value

def rounded_parts(left, right, groups):
    f32 = jnp.float32
    rows = left.shape[0]
    inner = left.shape[1] // groups
    parts = jnp.einsum('sgc,gcd->sgd', left.reshape(rows, groups, inner).astype(f32), right.reshape(groups, inner, right.shape[1]).astype(f32))
    parts = lax.optimization_barrier(parts.astype(jnp.bfloat16))
    return lax.optimization_barrier(jnp.sum(parts.astype(f32), axis=1))

def reference(tokens, norm_gain, w_query, w_key, w_value, w_outgate, w_igate, w_fgate, forget_bias, head_gain, w_proj, mixer_gain, w_gate, w_up, w_down, state_c, state_m, tail_keys, tail_values, tail_gate, block_forget, lengths):
    f32 = jnp.float32
    bf = jnp.bfloat16
    seqs = tokens.shape[0]
    xf = tokens.astype(f32)
    inv_first = lax.rsqrt(lax.optimization_barrier(jnp.mean(xf * xf, axis=1, keepdims=True)) + EPS)
    scaled = (xf * norm_gain).astype(bf)

    def project(weight):
        return jnp.dot(scaled, weight, preferred_element_type=f32) * inv_first
    query = project(w_query).reshape(seqs, HEADS, DH)
    key = project(w_key).reshape(seqs, HEADS, DH) * DH ** (-0.5)
    value = project(w_value).reshape(seqs, HEADS, DH)
    outgate = project(w_outgate)
    igate = project(w_igate)
    fpre = project(w_fgate) + forget_bias
    recalled = recall(query, key, value, igate, fpre, state_c, state_m, tail_keys, tail_values, tail_gate, block_forget, lengths)
    normed = recalled * lax.rsqrt(lax.optimization_barrier(jnp.mean(recalled * recalled, axis=2, keepdims=True)) + EPS)
    mixed = (normed.reshape(seqs, HEADS * DH) * head_gain * jax.nn.sigmoid(outgate)).astype(bf)
    attended = rounded_parts(mixed, w_proj, N_TP)
    middle = (xf + attended).astype(bf)
    middlef = middle.astype(f32)
    inv_second = lax.rsqrt(lax.optimization_barrier(jnp.mean(middlef * middlef, axis=1, keepdims=True)) + EPS)
    scaled_mid = (middlef * mixer_gain).astype(bf)
    gate = jnp.dot(scaled_mid, w_gate, preferred_element_type=f32) * inv_second
    up = jnp.dot(scaled_mid, w_up, preferred_element_type=f32) * inv_second
    hidden = (jax.nn.silu(gate) * up).astype(bf)
    mixed_out = rounded_parts(hidden, w_down, N_TP)
    return (middlef + mixed_out).astype(bf)
```

```python
import functools

import jax
import jax.numpy as jnp
from jax import lax
from jax.experimental import pallas as pl
from jax.experimental.pallas import tpu as pltpu
from jax.sharding import PartitionSpec as P

MESH = pl.DeviceIdType.MESH


def flip(pos, mask):
    out, bit = pos, 1
    while bit <= mask:
        if mask & bit:
            out = out + bit - 2 * bit * lax.rem(lax.div(pos, bit), 2)
        bit *= 2
    return out


def meet(axis, peers):
    barrier = pltpu.get_barrier_semaphore()
    for peer in peers:
        pl.semaphore_signal(barrier, inc=1, device_id={axis: peer}, device_id_type=MESH)
    pl.semaphore_wait(barrier, len(peers))


def send(src, dst, send_sem, recv_sem, axis, peer):
    copy = pltpu.make_async_remote_copy(
        src_ref=src,
        dst_ref=dst,
        send_sem=send_sem,
        recv_sem=recv_sem,
        device_id={axis: peer},
        device_id_type=MESH,
    )
    copy.start()
    return copy


def scatter_kernel(axis, outer, inner, jobs, count, *refs):
    f32 = jnp.float32
    ins, outs = refs[:count], refs[count : 2 * count]
    refs = refs[2 * count :]
    if inner > 1:
        recv1, refs = refs[:count], refs[count:]
        mid, refs = refs[:count], refs[count:]
    recv2, refs = refs[:count], refs[count:]
    if inner > 1:
        send1_sem, recv1_sem = refs[:2]
        refs = refs[2:]
    send2_sem, recv2_sem = refs
    me = lax.axis_index(axis)
    my_out, my_in = lax.div(me, inner), lax.rem(me, inner)
    in_peers = [flip(my_in, d) for d in range(1, inner)]
    out_peers = [flip(my_out, d) for d in range(1, outer)]
    meet(
        axis,
        [my_out * inner + p for p in in_peers] + [p * inner + my_in for p in out_peers],
    )
    first, second = [], []
    for j, (i, start, size) in enumerate(jobs):
        cols = pl.ds(start, size)
        first.append(
            [
                send(
                    ins[i].at[:, peer, :, cols],
                    recv1[i].at[d, :, :, cols],
                    send1_sem.at[j * (inner - 1) + d],
                    recv1_sem.at[j * (inner - 1) + d],
                    axis,
                    my_out * inner + peer,
                )
                for d, peer in enumerate(in_peers)
            ]
        )
    for j, (i, start, size) in enumerate(jobs):
        cols = pl.ds(start, size)
        for copy in first[j]:
            copy.wait_recv()
        if inner > 1:
            for z in range(outer):
                total = ins[i][z, my_in, :, cols].astype(f32)
                for d in range(inner - 1):
                    total = total + recv1[i][d, z, :, cols].astype(f32)
                mid[i][z, :, cols] = total.astype(mid[i].dtype)
        second.append(
            [
                send(
                    mid[i].at[peer, :, cols] if inner > 1 else ins[i].at[peer, 0, :, cols],
                    recv2[i].at[d, :, cols],
                    send2_sem.at[j * (outer - 1) + d],
                    recv2_sem.at[j * (outer - 1) + d],
                    axis,
                    peer * inner + my_in,
                )
                for d, peer in enumerate(out_peers)
            ]
        )
    for j, (i, start, size) in enumerate(jobs):
        cols = pl.ds(start, size)
        for copy in second[j]:
            copy.wait_recv()
        own = mid[i][my_out, :, cols] if inner > 1 else ins[i][my_out, 0, :, cols]
        total = own.astype(f32)
        for d in range(outer - 1):
            total = total + recv2[i][d, :, cols].astype(f32)
        outs[i][:, cols] = total
    for copies in first + second:
        for copy in copies:
            copy.wait_send()


def pieces(columns, most):
    tiles = columns // 128
    if columns % 128 or tiles == 0:
        return [(0, columns)]
    most = min(most, tiles)
    edges = [128 * (tiles * p // most) for p in range(most + 1)]
    return [(lo, hi - lo) for lo, hi in zip(edges, edges[1:])]


VMEM = pl.BlockSpec(memory_space=pltpu.VMEM)
LIMIT = 56 * 1024 * 1024


def scatter_sum(arrays, axis, outer, inner, most, ident):
    count = len(arrays)
    shapes = [a.shape[1:] for a in arrays]
    arrays = [a.reshape(outer, inner, *a.shape[1:]) for a in arrays]
    jobs = [(i, s, n) for i, (_, c) in enumerate(shapes) for s, n in pieces(c, most)]
    scratch = []
    if inner > 1:
        scratch += [pltpu.VMEM((inner - 1, outer, *s), a.dtype) for s, a in zip(shapes, arrays)]
        scratch += [pltpu.VMEM((outer, *s), a.dtype) for s, a in zip(shapes, arrays)]
    scratch += [pltpu.VMEM((outer - 1, *s), a.dtype) for s, a in zip(shapes, arrays)]
    if inner > 1:
        scratch += [pltpu.SemaphoreType.DMA((len(jobs) * (inner - 1),))] * 2
    scratch += [pltpu.SemaphoreType.DMA((len(jobs) * (outer - 1),))] * 2
    return pl.pallas_call(
        functools.partial(scatter_kernel, axis, outer, inner, jobs, count),
        out_shape=[jax.ShapeDtypeStruct(s, jnp.float32) for s in shapes],
        in_specs=[VMEM] * count,
        out_specs=[VMEM] * count,
        scratch_shapes=scratch,
        compiler_params=pltpu.CompilerParams(
            collective_id=ident, has_side_effects=True, vmem_limit_bytes=LIMIT
        ),
    )(*arrays)


def gather_kernel(axis, outer, inner, parts, x_ref, out_ref, *sems):
    out_send, out_recv = sems[:2]
    if inner > 1:
        in_send, in_recv = sems[2:4]
    own_sem = sems[-1]
    me = lax.axis_index(axis)
    my_out, my_in = lax.div(me, inner), lax.rem(me, inner)
    in_peers = [flip(my_in, d) for d in range(1, inner)]
    out_peers = [flip(my_out, d) for d in range(1, outer)]
    meet(
        axis,
        [my_out * inner + p for p in in_peers] + [p * inner + my_in for p in out_peers],
    )
    own = pltpu.make_async_copy(x_ref, out_ref.at[me], own_sem)
    own.start()
    across, along = [], []

    def pass_on(block, src, c, e):
        cols = pl.ds(*parts[c])
        for d, peer in enumerate(in_peers):
            k = (c * outer + e) * (inner - 1) + d
            along.append(
                send(
                    src,
                    out_ref.at[block, :, cols],
                    in_send.at[k],
                    in_recv.at[k],
                    axis,
                    my_out * inner + peer,
                )
            )

    for c, part in enumerate(parts):
        cols = pl.ds(*part)
        across.append(
            [
                send(
                    x_ref.at[:, cols],
                    out_ref.at[me, :, cols],
                    out_send.at[c * (outer - 1) + d],
                    out_recv.at[c * (outer - 1) + d],
                    axis,
                    peer * inner + my_in,
                )
                for d, peer in enumerate(out_peers)
            ]
        )
        pass_on(me, x_ref.at[:, cols], c, 0)
    for c, part in enumerate(parts):
        for d, peer in enumerate(out_peers):
            across[c][d].wait_recv()
            block = peer * inner + my_in
            pass_on(block, out_ref.at[block, :, pl.ds(*part)], c, d + 1)
    own.wait()
    for copy in along:
        copy.wait_recv()
    for copies in across + [along]:
        for copy in copies:
            copy.wait_send()


def gather(x, axis, outer, inner, most, ident):
    parts = pieces(x.shape[1], most)
    sems = [pltpu.SemaphoreType.DMA((len(parts) * (outer - 1),))] * 2
    if inner > 1:
        sems += [pltpu.SemaphoreType.DMA((len(parts) * outer * (inner - 1),))] * 2
    sems += [pltpu.SemaphoreType.DMA]
    return pl.pallas_call(
        functools.partial(gather_kernel, axis, outer, inner, parts),
        out_shape=jax.ShapeDtypeStruct((outer * inner, *x.shape), x.dtype),
        in_specs=[VMEM],
        out_specs=VMEM,
        scratch_shapes=sems,
        compiler_params=pltpu.CompilerParams(
            collective_id=ident, has_side_effects=True, vmem_limit_bytes=LIMIT
        ),
    )(x)


def middle_kernel(axis, n, part_ref, tok_ref, out_ref, recv, mine, *sems):
    f32 = jnp.float32
    send1, recv1, send2, recv2 = sems
    me = lax.axis_index(axis)
    peers = [flip(me, d) for d in range(1, n)]
    meet(axis, peers)
    first = [
        send(part_ref.at[peer], recv.at[d], send1.at[d], recv1.at[d], axis, peer)
        for d, peer in enumerate(peers)
    ]
    for copy in first:
        copy.wait_recv()
    total = part_ref[me].astype(f32)
    for d in range(n - 1):
        total = total + recv[d].astype(f32)
    mid = (tok_ref[...].astype(f32) + total).astype(out_ref.dtype)
    mine[...] = mid
    second = [
        send(mine, out_ref.at[me], send2.at[d], recv2.at[d], axis, peer)
        for d, peer in enumerate(peers)
    ]
    out_ref[me] = mid
    for copy in second:
        copy.wait_recv()
    for copy in first + second:
        copy.wait_send()


def middle_sum(partials, tokens, axis, ident):
    n = partials.shape[0]
    return pl.pallas_call(
        functools.partial(middle_kernel, axis, n),
        out_shape=jax.ShapeDtypeStruct(partials.shape, tokens.dtype),
        in_specs=[VMEM] * 2,
        out_specs=VMEM,
        scratch_shapes=[
            pltpu.VMEM((n - 1, *partials.shape[1:]), partials.dtype),
            pltpu.VMEM(partials.shape[1:], tokens.dtype),
        ]
        + [pltpu.SemaphoreType.DMA((n - 1,))] * 4,
        compiler_params=pltpu.CompilerParams(
            collective_id=ident, has_side_effects=True, vmem_limit_bytes=LIMIT
        ),
    )(partials, tokens)


D = 4096


EPS = 1e-06


def recall(
    query,
    key,
    value,
    igate,
    fpre,
    state_c,
    state_m,
    tail_keys,
    tail_values,
    tail_gate,
    block_forget,
    lengths,
):
    f32 = jnp.float32
    span = tail_keys.shape[2]
    head_dim = query.shape[2]
    running = block_forget + jax.nn.log_sigmoid(fpre)
    inter = running + state_m
    live = jnp.arange(span, dtype=jnp.int32)[None, :] < lengths[:, None]
    tail_log = jnp.where(live[:, None, :], running[:, :, None] + tail_gate, -jnp.inf)
    top = jnp.maximum(jnp.maximum(inter, jnp.max(tail_log, axis=2)), igate)
    w_inter = jnp.exp(inter - top)
    w_tail = jnp.exp(tail_log - top[:, :, None])
    w_own = jnp.exp(igate - top)
    scores = jnp.einsum("shpd,shd->shp", tail_keys.astype(f32), query) * head_dim ** (-0.5)
    own = jnp.sum(query * key, axis=2)
    memory = jnp.einsum("shvk,shk->shv", state_c, query)
    weighted = w_tail * scores
    return (
        w_inter[:, :, None] * memory
        + jnp.einsum("shp,shpv->shv", weighted, tail_values.astype(f32))
        + (w_own * own)[:, :, None] * value
    )


def per_device(
    n_kv,
    n_tp,
    tokens,
    norm_gain,
    w_query,
    w_key,
    w_value,
    w_outgate,
    w_igate,
    w_fgate,
    forget_bias,
    head_gain,
    w_proj,
    mixer_gain,
    w_gate,
    w_up,
    w_down,
    state_c,
    state_m,
    tail_keys,
    tail_values,
    tail_gate,
    block_forget,
    lengths,
):
    f32 = jnp.float32
    bf = jnp.bfloat16
    kv_pos = lax.axis_index("kv")
    tp_pos = lax.axis_index("tp")
    rows = norm_gain.shape[0]
    heads = forget_bias.shape[0]
    head_dim = tail_keys.shape[3]
    seq_dev = lengths.shape[0]
    width = heads * head_dim
    inner = n_kv // 4 if n_kv % 4 == 0 else 1
    outer = n_kv // inner
    seqs, own_cols = tokens.shape

    def join(blocks):
        return jnp.moveaxis(blocks, 0, 1).reshape(seqs, n_tp * own_cols)

    def split(whole):
        return jnp.moveaxis(whole.reshape(seqs, n_tp, own_cols), 1, 0)

    def by_owner(array):
        return array.reshape(n_kv, seq_dev, array.shape[1])

    wide = join(gather(tokens, "tp", n_tp, 1, 1, 0))
    widef = wide.astype(f32)
    scaled = (widef * norm_gain).astype(bf)

    def local_cols(weight):
        return lax.dynamic_slice(weight, (kv_pos * rows, tp_pos * heads), (rows, heads))

    gate_weights = jnp.concatenate([local_cols(w_igate), local_cols(w_fgate)], axis=1)
    joined = jnp.concatenate([w_query, w_key, w_value, w_outgate], axis=1)
    proj = jnp.dot(scaled, joined, preferred_element_type=f32)
    gates = jnp.dot(scaled, gate_weights, preferred_element_type=f32)
    part_sq1 = jnp.sum(widef * widef, axis=1, keepdims=True)
    gates = jnp.concatenate(
        [gates, part_sq1, jnp.zeros((seqs, 127 - 2 * heads), f32)], axis=1
    )
    gates, proj = scatter_sum(
        [by_owner(gates), by_owner(proj.astype(bf))], "kv", outer, inner, 6, 1
    )
    inv_first = lax.rsqrt(gates[:, 2 * heads : 2 * heads + 1] / D + EPS)
    proj = proj * inv_first
    gates = gates[:, : 2 * heads] * inv_first
    query = proj[:, :width].reshape(seq_dev, heads, head_dim)
    key = proj[:, width : 2 * width].reshape(seq_dev, heads, head_dim) * head_dim ** (-0.5)
    value = proj[:, 2 * width : 3 * width].reshape(seq_dev, heads, head_dim)
    outgate = proj[:, 3 * width :]
    igate = gates[:, :heads]
    fpre = gates[:, heads:] + forget_bias
    recalled = recall(
        query,
        key,
        value,
        igate,
        fpre,
        state_c,
        state_m,
        tail_keys,
        tail_values,
        tail_gate,
        block_forget,
        lengths,
    )
    normed = recalled * lax.rsqrt(jnp.mean(recalled * recalled, axis=2, keepdims=True) + EPS)
    mixed = (normed.reshape(seq_dev, width) * head_gain * jax.nn.sigmoid(outgate)).astype(bf)
    all_mixed = gather(mixed, "kv", outer, inner, 1, 2).reshape(seqs, width)
    partial_value = jnp.dot(all_mixed, w_proj, preferred_element_type=f32)
    middle = join(middle_sum(split(partial_value.astype(bf)), tokens, "tp", 3))
    middlef = middle.astype(f32)
    part_sq2 = jnp.sum(middlef * middlef, axis=1)
    scaled_mid = (middlef * mixer_gain).astype(bf)
    gate_part = jnp.dot(scaled_mid, w_gate, preferred_element_type=f32)
    up_part = jnp.dot(scaled_mid, w_up, preferred_element_type=f32)
    sq_wide = jnp.broadcast_to(part_sq2[:, None], (seqs, 128))
    sq_sh, gate_sh, up_sh = scatter_sum(
        [by_owner(sq_wide), by_owner(gate_part.astype(bf)), by_owner(up_part.astype(bf))],
        "kv",
        outer,
        inner,
        5,
        4,
    )
    sq_sh = sq_sh[:, 0]
    inv_second = lax.rsqrt(sq_sh / D + EPS)[:, None]
    hidden_sh = (jax.nn.silu(gate_sh * inv_second) * (up_sh * inv_second)).astype(bf)
    hidden = gather(hidden_sh, "kv", outer, inner, 4, 5).reshape(seqs, hidden_sh.shape[1])
    down_part = jnp.dot(hidden, w_down, preferred_element_type=f32)
    (down_sum,) = scatter_sum([split(down_part.astype(bf))], "tp", n_tp, 1, 1, 6)
    residual = lax.dynamic_slice_in_dim(middlef, tp_pos * own_cols, own_cols, 1)
    return (residual + down_sum).astype(bf)


def solution(mesh):
    return jax.shard_map(
        functools.partial(per_device, mesh.shape["kv"], mesh.shape["tp"]),
        mesh=mesh,
        in_specs=(
            P(None, ("kv", "tp")),
            P("kv"),
            P("kv", "tp"),
            P("kv", "tp"),
            P("kv", "tp"),
            P("kv", "tp"),
            P(),
            P(),
            P("tp"),
            P("tp"),
            P("tp", "kv"),
            P("kv"),
            P("kv", "tp"),
            P("kv", "tp"),
            P("tp", "kv"),
            P("kv", "tp", None, None),
            P("kv", "tp"),
            P("kv", "tp", None, None),
            P("kv", "tp", None, None),
            P("kv", "tp", None),
            P("kv", "tp"),
            P("kv"),
        ),
        out_specs=P(None, ("kv", "tp")),
        check_vma=False,
    )
```
